32 devices in a mesh: kv: 16 (over z, y, x), tp: 2 (over core).
Axes of the slice: x: 2, y: 2, z: 4, core: 2. Of those that a mesh axis runs over, the one named last changes fastest.
Arguments:
- tokens: bfloat16 [256, 2048], P('kv', 'tp'), may hold values from -20 to 20
- norm_gain: float32 [2048], replicated, may hold values from 0.1 to 1.9
- w_query: bfloat16 [2048, 1024], P(None, 'tp'), may hold values from -0.125 to 0.125
- w_key: bfloat16 [2048, 1024], P(None, 'tp'), may hold values from -0.125 to 0.125
- w_value: bfloat16 [2048, 1024], P(None, 'tp'), may hold values from -0.125 to 0.125
- w_outgate: bfloat16 [2048, 1024], P(None, 'tp'), may hold values from -0.125 to 0.125
- w_input_gate: bfloat16 [2048, 8], replicated, may hold values from -0.125 to 0.125
- w_forget_gate: bfloat16 [2048, 8], replicated, may hold values from -0.125 to 0.125
- memory: float32 [256, 8, 128, 128], P('kv', 'tp'), may hold values from -6 to 6
- normalizer: float32 [256, 8, 128], P('kv', 'tp'), may hold values from -6 to 6
- memory_max: float32 [256, 8], P('kv', 'tp'), may hold values from -2 to 300
- w_output: bfloat16 [1024, 2048], P(None, 'tp'), may hold values from -0.1875 to 0.1875
- ffn_gain: float32 [2048], P('tp'), may hold values from 0.1 to 1.9
- w_gate: bfloat16 [2048, 5632], P('tp', 'kv'), may hold values from -0.125 to 0.125
- w_up: bfloat16 [2048, 5632], P('tp', 'kv'), may hold values from -0.125 to 0.125
- w_down: bfloat16 [5632, 2048], P('kv', 'tp'), may hold values from -0.078125 to 0.078125
Outputs:
- result: bfloat16 [256, 2048], P('kv', 'tp')
- new_memory: float32 [256, 8, 128, 128], P('kv', 'tp')
- new_normalizer: float32 [256, 8, 128], P('kv', 'tp')
- new_max: float32 [256, 8], P('kv', 'tp')
The draws below stay inside these ranges and needn't reach their ends.
All inputs are finite; a program needn't handle non-finite values.
Results may differ from the reference program's by a relative error of at most 0.013.
Values may be sent and summed in bfloat16 or wider, within the bound.
A program may use at most 64 MiB of HBM per device.

```python
import jax
import jax.numpy as jnp
from jax import lax

D = 2048
HEADS = 8
HEAD_DIM = 128
INNER = 1024
FF = 5632
BATCH = 256


def draw_tokens(key, part):
    key_list = jax.random.split(jax.random.fold_in(key, 11), 3)
    col_pos = jnp.arange(D, dtype=jnp.float32) / (D - 1)
    col_jitter = jnp.exp(jax.random.uniform(key_list[2], (D,), jnp.float32, jnp.log(0.7), jnp.log(1.4)))
    base_draw = jnp.clip(jax.random.normal(key_list[0], (BATCH, D), jnp.float32), -4.0, 4.0)
    rise_curve = 0.6 * jnp.exp(col_pos * jnp.log(3.0))
    row_factor = jnp.exp(jax.random.uniform(key_list[1], (BATCH,), jnp.float32, jnp.log(0.5), jnp.log(2.0)))
    full_draw = base_draw * row_factor[:, None] * (rise_curve * col_jitter)[None, :]
    return jnp.clip(full_draw, -20.0, 20.0).astype(jnp.bfloat16)


def draw_memory_max(key, part):
    key_list = jax.random.split(jax.random.fold_in(key, 23), 1)
    base_draw = jax.random.uniform(key_list[0], (BATCH, HEADS), jnp.float32, -2.0, 2.0)
    return base_draw.astype(jnp.float32)


def shard_levels(own_key, extent, cuts, low, largest):
    loudness, own = 1.0, jax.random.fold_in(own_key, 6)
    for position, blocks in cuts:
        draws = jnp.exp(jax.random.uniform(jax.random.fold_in(own, position), (blocks,), jnp.float32, low / len(cuts), largest / len(cuts)))
        loudness = loudness * jnp.repeat(draws, extent[position] // blocks).reshape([-1 if axis == position else 1 for axis in range(len(extent))])
    return loudness


def scatter_about(rng, dims, scale, reach, pieces=(), held_as=jnp.bfloat16):
    drawn = scale * jax.random.normal(rng, dims, jnp.float32)
    if pieces:
        drawn = drawn * shard_levels(rng, dims, pieces, -0.22, 0.18)
    return jnp.clip(drawn, -reach, reach).astype(held_as)


def setup_inputs(seed: int = 0) -> dict:
    seeds = jax.random.split(jax.random.key(seed), 17)
    tokens = draw_tokens(jax.random.fold_in(seeds[16], 71), 0)
    norm_gain = jnp.clip(1.0 + 0.18 * jax.random.normal(seeds[1], (D,), jnp.float32), 0.1, 1.9)
    w_query = scatter_about(seeds[2], (D, INNER), D ** -0.5, 0.125, ((1, 2),))
    w_key = scatter_about(seeds[3], (D, INNER), D ** -0.5, 0.125, ((1, 2),))
    w_value = scatter_about(seeds[4], (D, INNER), D ** -0.5, 0.125, ((1, 2),))
    w_outgate = scatter_about(seeds[5], (D, INNER), D ** -0.5, 0.125, ((1, 2),))
    w_input_gate = scatter_about(seeds[6], (D, HEADS), D ** -0.5, 0.125)
    w_forget_gate = scatter_about(seeds[7], (D, HEADS), D ** -0.5, 0.125)
    memory = scatter_about(seeds[8], (BATCH, HEADS, HEAD_DIM, HEAD_DIM), 1.0, 6.0, ((0, 16), (1, 2)), jnp.float32)
    normalizer = scatter_about(seeds[9], (BATCH, HEADS, HEAD_DIM), 1.0, 6.0, ((0, 16), (1, 2)), jnp.float32)
    memory_max = draw_memory_max(jax.random.fold_in(seeds[16], 71), 0)
    w_output = scatter_about(seeds[11], (INNER, D), INNER ** -0.5, 0.1875, ((1, 2),))
    ffn_gain = jnp.clip(1.0 + 0.18 * jax.random.normal(seeds[12], (D,), jnp.float32), 0.1, 1.9)
    w_gate = scatter_about(seeds[13], (D, FF), D ** -0.5, 0.125, ((0, 2), (1, 16)))
    w_up = scatter_about(seeds[14], (D, FF), D ** -0.5, 0.125, ((0, 2), (1, 16)))
    w_down = scatter_about(seeds[15], (FF, D), FF ** -0.5, 0.078125, ((0, 16), (1, 2)))
    return dict(tokens=tokens, norm_gain=norm_gain, w_query=w_query, w_key=w_key, w_value=w_value, w_outgate=w_outgate, w_input_gate=w_input_gate, w_forget_gate=w_forget_gate, memory=memory, normalizer=normalizer, memory_max=memory_max, w_output=w_output, ffn_gain=ffn_gain, w_gate=w_gate, w_up=w_up, w_down=w_down)


def reference(tokens, norm_gain, w_query, w_key, w_value, w_outgate, w_input_gate, w_forget_gate, memory, normalizer, memory_max, w_output, ffn_gain, w_gate, w_up, w_down):
    tokens_f = tokens.astype(jnp.float32)
    row_scale = lax.rsqrt(lax.optimization_barrier(jnp.mean(tokens_f * tokens_f, axis=-1, keepdims=True)) + 1e-06)
    normed = (tokens_f * row_scale * norm_gain).astype(jnp.bfloat16)

    def project(weight):
        return jnp.dot(normed, weight, preferred_element_type=jnp.float32).reshape(BATCH, HEADS, HEAD_DIM)
    queries = project(w_query) * HEAD_DIM ** (-0.5)
    key_vec = project(w_key)
    values = project(w_value)
    outgate = project(w_outgate)
    igate = jnp.dot(normed, w_input_gate, preferred_element_type=jnp.float32)
    lforget = jax.nn.log_sigmoid(jnp.dot(normed, w_forget_gate, preferred_element_type=jnp.float32))
    new_max = jnp.maximum(lforget + memory_max, igate)
    keep_weight = jnp.exp(lforget + memory_max - new_max)
    admit_weight = jnp.exp(igate - new_max)
    new_memory = keep_weight[..., None, None] * memory + admit_weight[..., None, None] * (key_vec[..., :, None] * values[..., None, :])
    new_normalizer = keep_weight[..., None] * normalizer + admit_weight[..., None] * key_vec
    numerator = jnp.einsum('bhd,bhdv->bhv', queries, new_memory, precision=lax.Precision.HIGHEST)
    denominator = lax.optimization_barrier(jnp.sum(queries * new_normalizer, axis=-1))
    cell_out = numerator / jnp.maximum(jnp.abs(denominator), jnp.exp(-new_max))[..., None]
    head_mean = lax.optimization_barrier(jnp.mean(cell_out, axis=-1, keepdims=True))
    centered = cell_out - head_mean
    head_var = lax.optimization_barrier(jnp.mean(centered * centered, axis=-1, keepdims=True))
    mixed = (jax.nn.sigmoid(outgate) * centered * lax.rsqrt(head_var + 1e-05)).reshape(BATCH, INNER).astype(jnp.bfloat16)
    resid = (tokens_f + jnp.dot(mixed, w_output, preferred_element_type=jnp.float32)).astype(jnp.bfloat16)
    resid_f = resid.astype(jnp.float32)
    ffn_scale = lax.rsqrt(lax.optimization_barrier(jnp.mean(resid_f * resid_f, axis=-1, keepdims=True)) + 1e-06)
    ffn_in = (resid_f * ffn_gain).astype(jnp.bfloat16)
    gate_act = ffn_scale * jnp.dot(ffn_in, w_gate, preferred_element_type=jnp.float32)
    up_act = ffn_scale * jnp.dot(ffn_in, w_up, preferred_element_type=jnp.float32)
    hidden = (jax.nn.silu(gate_act) * up_act).astype(jnp.bfloat16)
    result = (resid_f + jnp.dot(hidden, w_down, preferred_element_type=jnp.float32)).astype(jnp.bfloat16)
    return (result, new_memory, new_normalizer, new_max)
```

```python
import functools

import jax
import jax.numpy as jnp
from jax import lax
from jax.experimental import pallas as pl
from jax.experimental.pallas import tpu as pltpu
from jax.sharding import PartitionSpec as P

F32, BF16 = jnp.float32, jnp.bfloat16
MESH = pl.DeviceIdType.MESH
ANY = pl.BlockSpec(memory_space=pl.ANY)
VMEM = pl.BlockSpec(memory_space=pltpu.VMEM)


def partner(index, bits):
    out, bit = index, 1
    while bit <= bits:
        if bits & bit:
            out = out + bit - 2 * bit * ((index // bit) % 2)
        bit *= 2
    return out


def split_groups(count):
    slow = 1
    while slow * slow < count:
        slow *= 2
    assert count % slow == 0
    return slow, count // slow


def greet(devices):
    barrier = pltpu.get_barrier_semaphore()
    for device in devices:
        pl.semaphore_signal(barrier, inc=1, device_id=device, device_id_type=MESH)
    pl.semaphore_wait(barrier, len(devices))


def mixer_kernel(
    nz, ny, nt, width,
    mixed_ref, tokens_ref, gain_ref, w_out_hbm, w_gate_hbm, w_up_hbm, w_down_hbm,
    out_ref,
    w_out, w_gate, w_up, w_down, mix, rows, part, part_in, down, down_in, total, total_in,
    load_sem, mix_sem, zed_sem, plane_sem, part_sem, down_sem, total_sem,
):
    k, t = lax.axis_index("kv"), lax.axis_index("tp")
    z, y = k // ny, k % ny
    own, cols = rows.shape[1], rows.shape[2]
    ff = w_down.shape[0]
    pad = (part.shape[2] - 128) // 2

    loads = [
        pltpu.make_async_copy(src, dst, load_sem.at[i])
        for i, (src, dst) in enumerate(
            ((w_out_hbm, w_out), (w_gate_hbm, w_gate), (w_up_hbm, w_up), (w_down_hbm, w_down))
        )
    ]
    for load in loads:
        load.start()

    def at_zed(off):
        return (partner(z, off) * ny + y, t)

    def at_plane(off):
        return (z * ny + partner(y, off), t)

    def at_tp(off):
        return (k, partner(t, off))

    greet(
        [at_tp(o) for o in range(1, nt)]
        + [at_plane(o) for o in range(1, ny)]
        + [at_zed(o) for o in range(1, nz)]
    )
    started = []

    def send(src, dst, sems, device):
        copy = pltpu.make_async_remote_copy(
            src_ref=src, dst_ref=dst, send_sem=sems.at[0], recv_sem=sems.at[1],
            device_id=device, device_id_type=MESH,
        )
        copy.start()
        started.append(copy)
        return copy

    mixes = [send(mixed_ref, mix.at[o - 1], mix_sem.at[o - 1], at_tp(o)) for o in range(1, nt)]
    loads[0].wait()
    inner = mixed_ref.shape[1]

    def project(value, owner):
        return jnp.dot(value, w_out[pl.ds(pl.multiple_of(owner * inner, inner), inner), :], preferred_element_type=F32)

    acc = tokens_ref[...].astype(F32) + project(mixed_ref[...], t)
    for o in range(1, nt):
        mixes[o - 1].wait_recv()
        acc = acc + project(mix[o - 1], partner(t, o))
    resid = acc.astype(BF16)
    rows[k] = resid

    zeds = {o: send(rows.at[k], rows.at[k], zed_sem.at[o], at_zed(o)) for o in range(1, nz)}
    planes = {}

    def spread(off):
        source = partner(z, off) * ny + y
        if off:
            zeds[off].wait_recv()
        for o in range(1, ny):
            planes[off, o] = send(rows.at[source], rows.at[source], plane_sem.at[off, o], at_plane(o))

    parts, gates, downs, totals, keep = {}, {}, {}, {}, {}

    def stage_a(off):
        for o in range(1, ny):
            planes[off, o].wait_recv()
        if off == 0:
            for load in loads[1:3]:
                load.wait()
        x = rows[pl.ds(partner(z, off) * ny, ny)].reshape(ny * own, cols)
        xf = x.astype(F32)
        square = jnp.sum(xf * xf, axis=-1, keepdims=True)
        h = (xf * gain_ref[...]).astype(BF16)
        gate = jnp.dot(h, w_gate[...], preferred_element_type=F32)
        up = jnp.dot(h, w_up[...], preferred_element_type=F32)
        high = square.astype(BF16).astype(F32)
        lane = lax.broadcasted_iota(jnp.int32, (ny * own, 128), 1)
        part[off, :, 0:ff] = gate.astype(BF16)
        part[off, :, pad : pad + ff] = up.astype(BF16)
        part[off, :, 2 * pad :] = jnp.where(lane < 64, high, square - high).astype(BF16)
        for o in range(1, nt):
            parts[off, o] = send(part.at[off], part_in.at[off, o - 1], part_sem.at[off, o - 1], at_tp(o))
        gates[off] = (gate, up, square)

    def stage_b(off):
        gate, up, square = gates.pop(off)
        for o in range(1, nt):
            parts[off, o].wait_recv()
            gate = gate + part_in[off, o - 1, :, 0:ff].astype(F32)
            up = up + part_in[off, o - 1, :, pad : pad + ff].astype(F32)
            tail = part_in[off, o - 1, :, 2 * pad :].astype(F32)
            square = square + jnp.sum(tail, axis=-1, keepdims=True) * (1.0 / 64)
        scale = lax.rsqrt(square / width + 1e-06)
        g = scale * gate
        hidden = (g / (1.0 + jnp.exp(-g)) * (scale * up)).astype(BF16)
        if off == 0:
            loads[3].wait()
        out = jnp.dot(hidden, w_down[...], preferred_element_type=F32)
        down[off] = out.reshape(ny, own, cols).astype(BF16)
        for o in range(1, ny):
            downs[off, o] = send(down.at[off, partner(y, o)], down_in.at[off, o - 1], down_sem.at[off, o], at_plane(o))

    def stage_c(off):
        acc = down[off, y].astype(F32)
        for o in range(1, ny):
            downs[off, o].wait_recv()
            acc = acc + down_in[off, o - 1].astype(F32)
        if off == 0:
            keep[0] = acc
        else:
            total[off] = acc.astype(BF16)
            totals[off] = send(total.at[off], total_in.at[off], total_sem.at[off], at_zed(off))

    spread(0)
    if nz > 1:
        spread(1)
    stage_a(0)
    for o in range(2, nz):
        spread(o)
    for o in range(0, nz + 2):
        if 1 <= o + 1 < nz:
            stage_a(o + 1)
        if o < nz:
            stage_b(o)
        if 0 <= o - 1 < nz:
            stage_c(o - 1)
    acc = rows[k].astype(F32) + keep[0]
    for o in range(1, nz):
        totals[o].wait_recv()
        acc = acc + total_in[o].astype(F32)
    out_ref[...] = acc.astype(BF16)
    for copy in started:
        copy.wait_send()


def channel_mixer(mesh, mixed, tokens, ffn_gain, w_output, w_gate, w_up, w_down):
    n, nt = mesh.shape["kv"], mesh.shape["tp"]
    nz, ny = split_groups(n)
    own, cols = tokens.shape
    ff = w_down.shape[0]
    pad = -(-ff // 128) * 128
    dma = pltpu.SemaphoreType.DMA
    peers = max(nt - 1, 1)
    return pl.pallas_call(
        functools.partial(mixer_kernel, nz, ny, nt, cols * nt),
        out_shape=jax.ShapeDtypeStruct((own, cols), BF16),
        in_specs=[VMEM, VMEM, VMEM, ANY, ANY, ANY, ANY],
        out_specs=VMEM,
        scratch_shapes=[
            pltpu.VMEM(w_output.shape, BF16),
            pltpu.VMEM(w_gate.shape, BF16),
            pltpu.VMEM(w_up.shape, BF16),
            pltpu.VMEM(w_down.shape, BF16),
            pltpu.VMEM((peers,) + mixed.shape, BF16),
            pltpu.VMEM((n, own, cols), BF16),
            pltpu.VMEM((nz, ny * own, 2 * pad + 128), BF16),
            pltpu.VMEM((nz, peers, ny * own, 2 * pad + 128), BF16),
            pltpu.VMEM((nz, ny, own, cols), BF16),
            pltpu.VMEM((nz, ny, own, cols), BF16),
            pltpu.VMEM((nz, own, cols), BF16),
            pltpu.VMEM((nz, own, cols), BF16),
            dma((4,)),
            dma((peers, 2)),
            dma((nz, 2)),
            dma((nz, ny, 2)),
            dma((nz, peers, 2)),
            dma((nz, ny, 2)),
            dma((nz, 2)),
        ],
        compiler_params=pltpu.CompilerParams(collective_id=0, has_side_effects=True),
        name="channel_mixer",
    )(mixed, tokens, ffn_gain.reshape(1, cols), w_output, w_gate, w_up, w_down)


def per_device(
    mesh,
    tokens,
    norm_gain,
    w_query,
    w_key,
    w_value,
    w_outgate,
    w_input_gate,
    w_forget_gate,
    memory,
    normalizer,
    memory_max,
    w_output,
    ffn_gain,
    w_gate,
    w_up,
    w_down,
):
    local_rows = tokens.shape[0]
    head_count = memory.shape[1]
    head_dim = memory.shape[2]
    full_rows = lax.all_gather(tokens, "tp", axis=1, tiled=True)
    rows_f = full_rows.astype(jnp.float32)
    row_scale = lax.rsqrt(jnp.mean(rows_f * rows_f, axis=-1, keepdims=True) + 1e-06)
    normed = (rows_f * row_scale * norm_gain).astype(jnp.bfloat16)

    def project(weight):
        return jnp.dot(normed, weight, preferred_element_type=jnp.float32).reshape(
            local_rows, head_count, head_dim
        )

    queries = project(w_query) * head_dim ** (-0.5)
    key_vec = project(w_key)
    values = project(w_value)
    outgate = project(w_outgate)
    first_head = lax.axis_index("tp") * head_count
    igate = lax.dynamic_slice_in_dim(
        jnp.dot(normed, w_input_gate, preferred_element_type=jnp.float32), first_head, head_count, 1
    )
    forget_pre = lax.dynamic_slice_in_dim(
        jnp.dot(normed, w_forget_gate, preferred_element_type=jnp.float32),
        first_head,
        head_count,
        1,
    )
    lforget = jax.nn.log_sigmoid(forget_pre)
    new_max = jnp.maximum(lforget + memory_max, igate)
    keep_weight = jnp.exp(lforget + memory_max - new_max)
    admit_weight = jnp.exp(igate - new_max)
    new_memory = keep_weight[..., None, None] * memory + admit_weight[..., None, None] * (
        key_vec[..., :, None] * values[..., None, :]
    )
    new_normalizer = keep_weight[..., None] * normalizer + admit_weight[..., None] * key_vec
    numerator = jnp.einsum("bhd,bhdv->bhv", queries, new_memory, precision=lax.Precision.HIGHEST)
    denominator = jnp.sum(queries * new_normalizer, axis=-1)
    cell_out = numerator / jnp.maximum(jnp.abs(denominator), jnp.exp(-new_max))[..., None]
    head_mean = jnp.mean(cell_out, axis=-1, keepdims=True)
    centered = cell_out - head_mean
    head_var = jnp.mean(centered * centered, axis=-1, keepdims=True)
    mixed = (
        (jax.nn.sigmoid(outgate) * centered * lax.rsqrt(head_var + 1e-05))
        .reshape(local_rows, head_count * head_dim)
        .astype(jnp.bfloat16)
    )
    result = channel_mixer(mesh, mixed, tokens, ffn_gain, w_output, w_gate, w_up, w_down)
    return (result, new_memory, new_normalizer, new_max)


def solution(mesh):
    placed = (
        P("kv", "tp"),
        P(),
        P(None, "tp"),
        P(None, "tp"),
        P(None, "tp"),
        P(None, "tp"),
        P(),
        P(),
        P("kv", "tp", None, None),
        P("kv", "tp", None),
        P("kv", "tp"),
        P(None, "tp"),
        P("tp"),
        P("tp", "kv"),
        P("tp", "kv"),
        P("kv", "tp"),
    )
    return jax.shard_map(
        functools.partial(per_device, mesh),
        mesh=mesh,
        in_specs=placed,
        out_specs=(P("kv", "tp"), P("kv", "tp", None, None), P("kv", "tp", None), P("kv", "tp")),
        check_vma=False,
    )
```

```python
import functools

import jax
import jax.numpy as jnp
from jax import lax
from jax.experimental import pallas as pl
from jax.experimental.pallas import tpu as pltpu
from jax.sharding import PartitionSpec as P

F32, BF16 = jnp.float32, jnp.bfloat16
MESH = pl.DeviceIdType.MESH
ANY = pl.BlockSpec(memory_space=pl.ANY)
VMEM = pl.BlockSpec(memory_space=pltpu.VMEM)
DEPTH = 4


def partner(index, bits):
    out, bit = index, 1
    while bit <= bits:
        if bits & bit:
            out = out + bit - 2 * bit * ((index // bit) % 2)
        bit *= 2
    return out


def split_groups(count):
    slow = 1
    while slow * slow < count:
        slow *= 2
    assert count % slow == 0
    return slow, count // slow


def greet(devices):
    barrier = pltpu.get_barrier_semaphore()
    for device in devices:
        pl.semaphore_signal(barrier, inc=1, device_id=device, device_id_type=MESH)
    pl.semaphore_wait(barrier, len(devices))


def nt_dot(a, b):
    return lax.dot_general(a, b, (((1,), (1,)), ((), ())), preferred_element_type=F32)


def step_kernel(
    nz, ny, nt, width,
    tokens_ref, norm_gain_ref, w_ig_ref, w_fg_ref, normalizer_ref, memory_max_ref, gain_ref,
    w_key_hbm, w_value_hbm, w_query_hbm, w_outgate_hbm, memory_hbm, w_out_hbm, w_gate_hbm, w_up_hbm, w_down_hbm,
    out_ref, aux_ref, new_max_ref,
    w_key, w_value, w_query, w_outgate, memory, w_out, w_gate, w_up, w_down,
    tok, normed, num, mixed_ref, mix, rows, part, part_in, down, down_in, total, total_in,
    load_sem, tok_sem, mix_sem, zed_sem, plane_sem, part_sem, down_sem, total_sem,
):
    k, t = lax.axis_index("kv"), lax.axis_index("tp")
    z, y = k // ny, k % ny
    own, cols = rows.shape[1], rows.shape[2]
    heads, dim = memory.shape[0], memory.shape[3]
    ff = w_down.shape[0]
    pad = (part.shape[2] - 128) // 2

    pairs = [(w_key_hbm, w_key), (w_value_hbm, w_value), (w_query_hbm, w_query), (w_outgate_hbm, w_outgate)]
    pairs += [(memory_hbm.at[:, h], memory.at[h]) for h in range(heads)]
    pairs += [(w_out_hbm, w_out), (w_gate_hbm, w_gate), (w_up_hbm, w_up), (w_down_hbm, w_down)]
    loads = [pltpu.make_async_copy(src, dst, load_sem.at[i]) for i, (src, dst) in enumerate(pairs)]
    for load in loads[:DEPTH]:
        load.start()

    def arrived(i):
        loads[i].wait()
        if i + DEPTH < len(loads):
            loads[i + DEPTH].start()

    def at_zed(off):
        return (partner(z, off) * ny + y, t)

    def at_plane(off):
        return (z * ny + partner(y, off), t)

    def at_tp(off):
        return (k, partner(t, off))

    greet(
        [at_tp(o) for o in range(1, nt)]
        + [at_plane(o) for o in range(1, ny)]
        + [at_zed(o) for o in range(1, nz)]
    )
    started = []

    def send(src, dst, sems, device):
        copy = pltpu.make_async_remote_copy(
            src_ref=src, dst_ref=dst, send_sem=sems.at[0], recv_sem=sems.at[1],
            device_id=device, device_id_type=MESH,
        )
        copy.start()
        started.append(copy)
        return copy

    toks = [send(tokens_ref, tok.at[o - 1], tok_sem.at[o - 1], at_tp(o)) for o in range(1, nt)]
    blocks = [(t, tokens_ref[...].astype(F32))]
    for o in range(1, nt):
        toks[o - 1].wait_recv()
        blocks.append((partner(t, o), tok[o - 1].astype(F32)))
    square = blocks[0][1] * blocks[0][1]
    square = jnp.sum(square, axis=-1, keepdims=True)
    for _, block in blocks[1:]:
        square = square + jnp.sum(block * block, axis=-1, keepdims=True)
    row_scale = lax.rsqrt(square / width + 1e-06)
    for owner, block in blocks:
        at = pl.ds(pl.multiple_of(owner * cols, cols), cols)
        normed[:, at] = (block * row_scale * norm_gain_ref[:, at]).astype(BF16)
    x = normed[...]
    igates, fgates = nt_dot(x, w_ig_ref[...]), nt_dot(x, w_fg_ref[...])

    def projected(i, weight):
        arrived(i)
        return jnp.dot(x, weight[...], preferred_element_type=F32)

    keys = projected(0, w_key)
    values = projected(1, w_value)
    queries = projected(2, w_query) * dim ** (-0.5)
    outgates = projected(3, w_outgate)
    lane = lax.broadcasted_iota(jnp.int32, igates.shape, 1)
    for h in range(heads):
        mine = lane == t * heads + h
        igate = jnp.sum(jnp.where(mine, igates, 0.0), axis=-1, keepdims=True)
        forget = jnp.sum(jnp.where(mine, fgates, 0.0), axis=-1, keepdims=True)
        carried = jnp.minimum(forget, 0.0) - jnp.log1p(jnp.exp(-jnp.abs(forget))) + memory_max_ref[:, h : h + 1]
        new_max = jnp.maximum(carried, igate)
        keep_weight = jnp.exp(carried - new_max)
        new_max_ref[:, h : h + 1] = new_max
        at = slice(h * dim, (h + 1) * dim)
        key, value, query = jnp.exp(igate - new_max) * keys[:, at], values[:, at], queries[:, at]
        keep_wide = jnp.broadcast_to(keep_weight, key.shape)
        aux_ref[0, h], aux_ref[1, h], aux_ref[2, h] = keep_wide, key, value
        denominator = jnp.sum(query * (keep_wide * normalizer_ref[:, h, :] + key), axis=-1, keepdims=True)
        match = jnp.sum(query * key, axis=-1, keepdims=True)
        turned = query.T
        arrived(4 + h)
        for r in range(own):
            num[r : r + 1, :] = jnp.sum(memory[h, r] * turned[:, r : r + 1], axis=0, keepdims=True)
        numerator = keep_wide * num[...] + match * value
        cell_out = numerator / jnp.maximum(jnp.abs(denominator), jnp.exp(-new_max))
        centered = cell_out - jnp.mean(cell_out, axis=-1, keepdims=True)
        head_var = jnp.mean(centered * centered, axis=-1, keepdims=True)
        gate = 1.0 / (1.0 + jnp.exp(-outgates[:, at]))
        mixed_ref[:, at] = (gate * centered * lax.rsqrt(head_var + 1e-05)).astype(BF16)

    mixes = [send(mixed_ref, mix.at[o - 1], mix_sem.at[o - 1], at_tp(o)) for o in range(1, nt)]
    first = 4 + heads
    arrived(first)
    inner = mixed_ref.shape[1]

    def project(value, owner):
        return jnp.dot(value, w_out[pl.ds(pl.multiple_of(owner * inner, inner), inner), :], preferred_element_type=F32)

    acc = tokens_ref[...].astype(F32) + project(mixed_ref[...], t)
    for o in range(1, nt):
        mixes[o - 1].wait_recv()
        acc = acc + project(mix[o - 1], partner(t, o))
    rows[k] = acc.astype(BF16)

    zeds = {o: send(rows.at[k], rows.at[k], zed_sem.at[o], at_zed(o)) for o in range(1, nz)}
    planes = {}

    def spread(off):
        source = partner(z, off) * ny + y
        if off:
            zeds[off].wait_recv()
        for o in range(1, ny):
            planes[off, o] = send(rows.at[source], rows.at[source], plane_sem.at[off, o], at_plane(o))

    parts, gates, downs, totals, keep = {}, {}, {}, {}, {}

    def stage_a(off):
        for o in range(1, ny):
            planes[off, o].wait_recv()
        if off == 0:
            arrived(first + 1)
            arrived(first + 2)
        x = rows[pl.ds(partner(z, off) * ny, ny)].reshape(ny * own, cols)
        xf = x.astype(F32)
        square = jnp.sum(xf * xf, axis=-1, keepdims=True)
        h = (xf * gain_ref[...]).astype(BF16)
        gate = nt_dot(h, w_gate[...])
        up = nt_dot(h, w_up[...])
        high = square.astype(BF16).astype(F32)
        lane = lax.broadcasted_iota(jnp.int32, (ny * own, 128), 1)
        part[off, :, 0:ff] = gate.astype(BF16)
        part[off, :, pad : pad + ff] = up.astype(BF16)
        part[off, :, 2 * pad :] = jnp.where(lane < 64, high, square - high).astype(BF16)
        for o in range(1, nt):
            parts[off, o] = send(part.at[off], part_in.at[off, o - 1], part_sem.at[off, o - 1], at_tp(o))
        gates[off] = (gate, up, square)

    def stage_b(off):
        gate, up, square = gates.pop(off)
        for o in range(1, nt):
            parts[off, o].wait_recv()
            gate = gate + part_in[off, o - 1, :, 0:ff].astype(F32)
            up = up + part_in[off, o - 1, :, pad : pad + ff].astype(F32)
            tail = part_in[off, o - 1, :, 2 * pad :].astype(F32)
            square = square + jnp.sum(tail, axis=-1, keepdims=True) * (1.0 / 64)
        scale = lax.rsqrt(square / width + 1e-06)
        g = scale * gate
        hidden = (g / (1.0 + jnp.exp(-g)) * (scale * up)).astype(BF16)
        if off == 0:
            arrived(first + 3)
        out = jnp.dot(hidden, w_down[...], preferred_element_type=F32)
        down[off] = out.reshape(ny, own, cols).astype(BF16)
        for o in range(1, ny):
            downs[off, o] = send(down.at[off, partner(y, o)], down_in.at[off, o - 1], down_sem.at[off, o], at_plane(o))

    def stage_c(off):
        acc = down[off, y].astype(F32)
        for o in range(1, ny):
            downs[off, o].wait_recv()
            acc = acc + down_in[off, o - 1].astype(F32)
        if off == 0:
            keep[0] = acc
        else:
            total[off] = acc.astype(BF16)
            totals[off] = send(total.at[off], total_in.at[off], total_sem.at[off], at_zed(off))

    spread(0)
    if nz > 1:
        spread(1)
    stage_a(0)
    for o in range(2, nz):
        spread(o)
    for o in range(0, nz + 2):
        if 1 <= o + 1 < nz:
            stage_a(o + 1)
        if o < nz:
            stage_b(o)
        if 0 <= o - 1 < nz:
            stage_c(o - 1)
    acc = rows[k].astype(F32) + keep[0]
    for o in range(1, nz):
        totals[o].wait_recv()
        acc = acc + total_in[o].astype(F32)
    out_ref[...] = acc.astype(BF16)
    for copy in started:
        copy.wait_send()


def update_kernel(chunk, memory_hbm, aux_ref, normalizer_ref, new_max_in, result_in, new_memory_hbm, new_norm_ref, new_max_ref, result_ref, memory, in_sem, out_sem):
    rows, heads = memory.shape[0], memory.shape[1]
    steps = range(rows // chunk)
    at = [pl.ds(i * chunk, chunk) for i in steps]
    loads = [pltpu.make_async_copy(memory_hbm.at[at[i]], memory.at[at[i]], in_sem.at[i]) for i in steps]
    stores = [pltpu.make_async_copy(memory.at[at[i]], new_memory_hbm.at[at[i]], out_sem.at[i]) for i in steps]
    for load in loads:
        load.start()
    turned = []
    for h in range(heads):
        new_norm_ref[:, h, :] = aux_ref[0, h] * normalizer_ref[:, h, :] + aux_ref[1, h]
        turned.append(aux_ref[1, h].T)
    new_max_ref[...] = new_max_in[...]
    result_ref[...] = result_in[...]
    for i in steps:
        loads[i].wait()
        for r in range(i * chunk, (i + 1) * chunk):
            for h in range(heads):
                memory[r, h] = aux_ref[0, h, r : r + 1, :] * memory[r, h] + turned[h][:, r : r + 1] * aux_ref[2, h, r : r + 1, :]
        stores[i].start()
    for store in stores:
        store.wait()


def per_device(
    mesh, tokens, norm_gain, w_query, w_key, w_value, w_outgate, w_input_gate, w_forget_gate,
    memory, normalizer, memory_max, w_output, ffn_gain, w_gate, w_up, w_down,
):
    n, nt = mesh.shape["kv"], mesh.shape["tp"]
    nz, ny = split_groups(n)
    own, cols = tokens.shape
    heads, dim = memory.shape[1], memory.shape[2]
    inner = heads * dim
    ff = w_down.shape[0]
    pad = -(-ff // 128) * 128
    dma = pltpu.SemaphoreType.DMA
    peers = max(nt - 1, 1)
    w_gate, w_up = w_gate.T, w_up.T
    vm = lambda like: pltpu.VMEM(like.shape, like.dtype)
    result, aux, new_max = pl.pallas_call(
        functools.partial(step_kernel, nz, ny, nt, cols * nt),
        out_shape=(
            jax.ShapeDtypeStruct((own, cols), BF16),
            jax.ShapeDtypeStruct((3, heads, own, dim), F32),
            jax.ShapeDtypeStruct((own, heads), F32),
        ),
        in_specs=[VMEM] * 7 + [ANY] * 9,
        out_specs=(VMEM, VMEM, VMEM),
        scratch_shapes=[
            vm(w_key), vm(w_value), vm(w_query), vm(w_outgate),
            pltpu.VMEM((heads, own, dim, dim), F32),
            vm(w_output), vm(w_gate), vm(w_up), vm(w_down),
            pltpu.VMEM((peers, own, cols), BF16),
            pltpu.VMEM((own, cols * nt), BF16),
            pltpu.VMEM((own, dim), F32),
            pltpu.VMEM((own, inner), BF16),
            pltpu.VMEM((peers, own, inner), BF16),
            pltpu.VMEM((n, own, cols), BF16),
            pltpu.VMEM((nz, ny * own, 2 * pad + 128), BF16),
            pltpu.VMEM((nz, peers, ny * own, 2 * pad + 128), BF16),
            pltpu.VMEM((nz, ny, own, cols), BF16),
            pltpu.VMEM((nz, ny, own, cols), BF16),
            pltpu.VMEM((nz, own, cols), BF16),
            pltpu.VMEM((nz, own, cols), BF16),
            dma((8 + heads,)),
            dma((peers, 2)),
            dma((peers, 2)),
            dma((nz, 2)),
            dma((nz, ny, 2)),
            dma((nz, peers, 2)),
            dma((nz, ny, 2)),
            dma((nz, 2)),
        ],
        compiler_params=pltpu.CompilerParams(collective_id=0, has_side_effects=True),
        name="decode_step",
    )(
        tokens, norm_gain.reshape(1, -1), w_input_gate.T, w_forget_gate.T, normalizer, memory_max,
        ffn_gain.reshape(1, cols), w_key, w_value, w_query, w_outgate, memory, w_output, w_gate, w_up, w_down,
    )
    chunk = 2 if own % 2 == 0 else 1
    new_memory, new_normalizer, new_max, result = pl.pallas_call(
        functools.partial(update_kernel, chunk),
        out_shape=(
            jax.ShapeDtypeStruct(memory.shape, F32),
            jax.ShapeDtypeStruct(normalizer.shape, F32),
            jax.ShapeDtypeStruct(memory_max.shape, F32),
            jax.ShapeDtypeStruct(tokens.shape, BF16),
        ),
        in_specs=[ANY, VMEM, VMEM, VMEM, VMEM],
        out_specs=(ANY, VMEM, VMEM, VMEM),
        scratch_shapes=[vm(memory), dma((own // chunk,)), dma((own // chunk,))],
        name="memory_update",
    )(memory, aux, normalizer, new_max, result)
    return (result, new_memory, new_normalizer, new_max)


def solution(mesh):
    placed = (
        P("kv", "tp"),
        P(),
        P(None, "tp"),
        P(None, "tp"),
        P(None, "tp"),
        P(None, "tp"),
        P(),
        P(),
        P("kv", "tp", None, None),
        P("kv", "tp", None),
        P("kv", "tp"),
        P(None, "tp"),
        P("tp"),
        P("tp", "kv"),
        P("tp", "kv"),
        P("kv", "tp"),
    )
    return jax.shard_map(
        functools.partial(per_device, mesh),
        mesh=mesh,
        in_specs=placed,
        out_specs=(P("kv", "tp"), P("kv", "tp", None, None), P("kv", "tp", None), P("kv", "tp")),
        check_vma=False,
    )
```

```python
import functools

import jax
import jax.numpy as jnp
from jax import lax
from jax.experimental import pallas as pl
from jax.experimental.pallas import tpu as pltpu
from jax.sharding import PartitionSpec as P

F32, BF16 = jnp.float32, jnp.bfloat16
MESH = pl.DeviceIdType.MESH
ANY = pl.BlockSpec(memory_space=pl.ANY)
VMEM = pl.BlockSpec(memory_space=pltpu.VMEM)
DEPTH = 4


def partner(index, bits):
    out, bit = index, 1
    while bit <= bits:
        if bits & bit:
            out = out + bit - 2 * bit * ((index // bit) % 2)
        bit *= 2
    return out


def split_groups(count):
    slow = 1
    while slow * slow < count:
        slow *= 2
    assert count % slow == 0
    return slow, count // slow


def greet(devices):
    barrier = pltpu.get_barrier_semaphore()
    for device in devices:
        pl.semaphore_signal(barrier, inc=1, device_id=device, device_id_type=MESH)
    pl.semaphore_wait(barrier, len(devices))


def nt_dot(a, b):
    return lax.dot_general(a, b, (((1,), (1,)), ((), ())), preferred_element_type=F32)


def step_kernel(
    nz, ny, nt, width,
    tokens_ref, norm_gain_ref, w_ig_ref, w_fg_ref, normalizer_ref, memory_max_ref, gain_ref,
    w_key_hbm, w_value_hbm, w_query_hbm, w_outgate_hbm, memory_hbm, w_out_hbm, w_gate_hbm, w_up_hbm, w_down_hbm,
    out_ref, aux_ref, new_max_ref,
    w_key, w_value, w_query, w_outgate, memory, w_out, w_gate, w_up, w_down,
    tok, normed, num, mixed_ref, mix, rows, part, part_in, down, down_in, total, total_in,
    load_sem, tok_sem, mix_sem, zed_sem, plane_sem, part_sem, down_sem, total_sem,
):
    k, t = lax.axis_index("kv"), lax.axis_index("tp")
    z, y = k // ny, k % ny
    own, cols = rows.shape[1], rows.shape[2]
    heads, dim = memory.shape[0], memory.shape[3]
    ff = w_down.shape[0]
    pad = (part.shape[2] - 128) // 2

    pairs = [(w_key_hbm, w_key), (w_value_hbm, w_value), (w_query_hbm, w_query), (w_outgate_hbm, w_outgate)]
    pairs += [(memory_hbm.at[:, h], memory.at[h]) for h in range(heads)]
    pairs += [(w_out_hbm, w_out), (w_gate_hbm, w_gate), (w_up_hbm, w_up), (w_down_hbm, w_down)]
    loads = [pltpu.make_async_copy(src, dst, load_sem.at[i]) for i, (src, dst) in enumerate(pairs)]
    for load in loads[:DEPTH]:
        load.start()

    def arrived(i):
        loads[i].wait()
        if i + DEPTH < len(loads):
            loads[i + DEPTH].start()

    def at_zed(off):
        return (partner(z, off) * ny + y, t)

    def at_plane(off):
        return (z * ny + partner(y, off), t)

    def at_tp(off):
        return (k, partner(t, off))

    greet(
        [at_tp(o) for o in range(1, nt)]
        + [at_plane(o) for o in range(1, ny)]
        + [at_zed(o) for o in range(1, nz)]
    )
    started = []

    def send(src, dst, sems, device):
        copy = pltpu.make_async_remote_copy(
            src_ref=src, dst_ref=dst, send_sem=sems.at[0], recv_sem=sems.at[1],
            device_id=device, device_id_type=MESH,
        )
        copy.start()
        started.append(copy)
        return copy

    toks = [send(tokens_ref, tok.at[o - 1], tok_sem.at[o - 1], at_tp(o)) for o in range(1, nt)]
    blocks = [(t, tokens_ref[...].astype(F32))]
    for o in range(1, nt):
        toks[o - 1].wait_recv()
        blocks.append((partner(t, o), tok[o - 1].astype(F32)))
    square = blocks[0][1] * blocks[0][1]
    square = jnp.sum(square, axis=-1, keepdims=True)
    for _, block in blocks[1:]:
        square = square + jnp.sum(block * block, axis=-1, keepdims=True)
    row_scale = lax.rsqrt(square / width + 1e-06)
    for owner, block in blocks:
        at = pl.ds(pl.multiple_of(owner * cols, cols), cols)
        normed[:, at] = (block * row_scale * norm_gain_ref[:, at]).astype(BF16)
    x = normed[...]
    igates, fgates = nt_dot(x, w_ig_ref[...]), nt_dot(x, w_fg_ref[...])

    def projected(i, weight):
        arrived(i)
        return jnp.dot(x, weight[...], preferred_element_type=F32)

    keys = projected(0, w_key)
    values = projected(1, w_value)
    queries = projected(2, w_query) * dim ** (-0.5)
    outgates = projected(3, w_outgate)
    lane = lax.broadcasted_iota(jnp.int32, igates.shape, 1)
    diagonal = lax.broadcasted_iota(jnp.int32, (own, own), 0) == lax.broadcasted_iota(jnp.int32, (own, own), 1)
    for h in range(heads):
        mine = lane == t * heads + h
        igate = jnp.sum(jnp.where(mine, igates, 0.0), axis=-1, keepdims=True)
        forget = jnp.sum(jnp.where(mine, fgates, 0.0), axis=-1, keepdims=True)
        carried = jnp.minimum(forget, 0.0) - jnp.log1p(jnp.exp(-jnp.abs(forget)))
        carried = carried + jnp.sum(jnp.where(diagonal, memory_max_ref[h : h + 1, :], 0.0), axis=-1, keepdims=True)
        new_max = jnp.maximum(carried, igate)
        keep_weight = jnp.exp(carried - new_max)
        new_max_ref[h : h + 1, :] = jnp.sum(jnp.where(diagonal, new_max, 0.0), axis=0, keepdims=True)
        at = slice(h * dim, (h + 1) * dim)
        key, value, query = jnp.exp(igate - new_max) * keys[:, at], values[:, at], queries[:, at]
        keep_wide = jnp.broadcast_to(keep_weight, key.shape)
        aux_ref[0, h], aux_ref[1, h], aux_ref[2, h] = keep_wide, key, value
        denominator = jnp.sum(query * (keep_wide * normalizer_ref[:, h, :] + key), axis=-1, keepdims=True)
        match = jnp.sum(query * key, axis=-1, keepdims=True)
        turned = query.T
        arrived(4 + h)
        for r in range(own):
            num[r : r + 1, :] = jnp.sum(memory[h, r] * turned[:, r : r + 1], axis=0, keepdims=True)
        numerator = keep_wide * num[...] + match * value
        cell_out = numerator / jnp.maximum(jnp.abs(denominator), jnp.exp(-new_max))
        centered = cell_out - jnp.mean(cell_out, axis=-1, keepdims=True)
        head_var = jnp.mean(centered * centered, axis=-1, keepdims=True)
        gate = 1.0 / (1.0 + jnp.exp(-outgates[:, at]))
        mixed_ref[:, at] = (gate * centered * lax.rsqrt(head_var + 1e-05)).astype(BF16)

    mixes = [send(mixed_ref, mix.at[o - 1], mix_sem.at[o - 1], at_tp(o)) for o in range(1, nt)]
    first = 4 + heads
    arrived(first)
    inner = mixed_ref.shape[1]

    def project(value, owner):
        return jnp.dot(value, w_out[pl.ds(pl.multiple_of(owner * inner, inner), inner), :], preferred_element_type=F32)

    acc = tokens_ref[...].astype(F32) + project(mixed_ref[...], t)
    for o in range(1, nt):
        mixes[o - 1].wait_recv()
        acc = acc + project(mix[o - 1], partner(t, o))
    rows[k] = acc.astype(BF16)

    zeds = {o: send(rows.at[k], rows.at[k], zed_sem.at[o], at_zed(o)) for o in range(1, nz)}
    planes = {}

    def spread(off):
        source = partner(z, off) * ny + y
        if off:
            zeds[off].wait_recv()
        for o in range(1, ny):
            planes[off, o] = send(rows.at[source], rows.at[source], plane_sem.at[off, o], at_plane(o))

    parts, gates, downs, totals, keep = {}, {}, {}, {}, {}

    def stage_a(off):
        for o in range(1, ny):
            planes[off, o].wait_recv()
        if off == 0:
            arrived(first + 1)
            arrived(first + 2)
        x = rows[pl.ds(partner(z, off) * ny, ny)].reshape(ny * own, cols)
        xf = x.astype(F32)
        square = jnp.sum(xf * xf, axis=-1, keepdims=True)
        h = (xf * gain_ref[...]).astype(BF16)
        gate = nt_dot(h, w_gate[...])
        up = nt_dot(h, w_up[...])
        high = square.astype(BF16).astype(F32)
        lane = lax.broadcasted_iota(jnp.int32, (ny * own, 128), 1)
        part[off, :, 0:ff] = gate.astype(BF16)
        part[off, :, pad : pad + ff] = up.astype(BF16)
        part[off, :, 2 * pad :] = jnp.where(lane < 64, high, square - high).astype(BF16)
        for o in range(1, nt):
            parts[off, o] = send(part.at[off], part_in.at[off, o - 1], part_sem.at[off, o - 1], at_tp(o))
        gates[off] = (gate, up, square)

    def stage_b(off):
        gate, up, square = gates.pop(off)
        for o in range(1, nt):
            parts[off, o].wait_recv()
            gate = gate + part_in[off, o - 1, :, 0:ff].astype(F32)
            up = up + part_in[off, o - 1, :, pad : pad + ff].astype(F32)
            tail = part_in[off, o - 1, :, 2 * pad :].astype(F32)
            square = square + jnp.sum(tail, axis=-1, keepdims=True) * (1.0 / 64)
        scale = lax.rsqrt(square / width + 1e-06)
        g = scale * gate
        hidden = (g / (1.0 + jnp.exp(-g)) * (scale * up)).astype(BF16)
        if off == min(1, nz - 1):
            arrived(first + 3)
        out = jnp.dot(hidden, w_down[...], preferred_element_type=F32)
        down[off] = out.reshape(ny, own, cols).astype(BF16)
        for o in range(1, ny):
            downs[off, o] = send(down.at[off, partner(y, o)], down_in.at[off, o - 1], down_sem.at[off, o], at_plane(o))

    def stage_c(off):
        acc = down[off, y].astype(F32)
        for o in range(1, ny):
            downs[off, o].wait_recv()
            acc = acc + down_in[off, o - 1].astype(F32)
        if off == 0:
            keep[0] = acc
        else:
            total[off] = acc.astype(BF16)
            totals[off] = send(total.at[off], total_in.at[off], total_sem.at[off], at_zed(off))

    spread(0)
    if nz > 1:
        spread(1)
    stage_a(0)
    for o in range(2, nz):
        spread(o)
    for o in range(1, nz + 1):
        if o < nz:
            stage_a(o)
        if o > 1:
            stage_b(o - 1)
        if o > 2:
            stage_c(o - 2)
    stage_b(0)
    if nz > 1:
        stage_c(nz - 1)
    stage_c(0)
    acc = rows[k].astype(F32) + keep[0]
    for o in range(1, nz):
        totals[o].wait_recv()
        acc = acc + total_in[o].astype(F32)
    out_ref[...] = acc.astype(BF16)
    for copy in started:
        copy.wait_send()


def update_kernel(chunk, memory_hbm, aux_ref, normalizer_ref, new_max_in, result_in, new_memory_hbm, new_norm_ref, new_max_ref, result_ref, memory, in_sem, out_sem):
    rows, heads = memory.shape[0], memory.shape[1]
    steps = range(rows // chunk)
    at = [pl.ds(i * chunk, chunk) for i in steps]
    loads = [pltpu.make_async_copy(memory_hbm.at[at[i]], memory.at[at[i]], in_sem.at[i]) for i in steps]
    stores = [pltpu.make_async_copy(memory.at[at[i]], new_memory_hbm.at[at[i]], out_sem.at[i]) for i in steps]
    for load in loads:
        load.start()
    turned = []
    for h in range(heads):
        new_norm_ref[:, h, :] = aux_ref[0, h] * normalizer_ref[:, h, :] + aux_ref[1, h]
        turned.append(aux_ref[1, h].T)
    new_max_ref[...] = new_max_in[...]
    result_ref[...] = result_in[...]
    for i in steps:
        loads[i].wait()
        for r in range(i * chunk, (i + 1) * chunk):
            for h in range(heads):
                memory[r, h] = aux_ref[0, h, r : r + 1, :] * memory[r, h] + turned[h][:, r : r + 1] * aux_ref[2, h, r : r + 1, :]
        stores[i].start()
    for store in stores:
        store.wait()


def per_device(
    mesh, tokens, norm_gain, w_query, w_key, w_value, w_outgate, w_input_gate, w_forget_gate,
    memory, normalizer, memory_max, w_output, ffn_gain, w_gate, w_up, w_down,
):
    n, nt = mesh.shape["kv"], mesh.shape["tp"]
    nz, ny = split_groups(n)
    own, cols = tokens.shape
    heads, dim = memory.shape[1], memory.shape[2]
    inner = heads * dim
    ff = w_down.shape[0]
    pad = -(-ff // 128) * 128
    dma = pltpu.SemaphoreType.DMA
    peers = max(nt - 1, 1)
    w_gate, w_up = w_gate.T, w_up.T
    vm = lambda like: pltpu.VMEM(like.shape, like.dtype)
    result, aux, new_max = pl.pallas_call(
        functools.partial(step_kernel, nz, ny, nt, cols * nt),
        out_shape=(
            jax.ShapeDtypeStruct((own, cols), BF16),
            jax.ShapeDtypeStruct((3, heads, own, dim), F32),
            jax.ShapeDtypeStruct((heads, own), F32),
        ),
        in_specs=[VMEM] * 7 + [ANY] * 9,
        out_specs=(VMEM, VMEM, VMEM),
        scratch_shapes=[
            vm(w_key), vm(w_value), vm(w_query), vm(w_outgate),
            pltpu.VMEM((heads, own, dim, dim), F32),
            vm(w_output), vm(w_gate), vm(w_up), vm(w_down),
            pltpu.VMEM((peers, own, cols), BF16),
            pltpu.VMEM((own, cols * nt), BF16),
            pltpu.VMEM((own, dim), F32),
            pltpu.VMEM((own, inner), BF16),
            pltpu.VMEM((peers, own, inner), BF16),
            pltpu.VMEM((n, own, cols), BF16),
            pltpu.VMEM((nz, ny * own, 2 * pad + 128), BF16),
            pltpu.VMEM((nz, peers, ny * own, 2 * pad + 128), BF16),
            pltpu.VMEM((nz, ny, own, cols), BF16),
            pltpu.VMEM((nz, ny, own, cols), BF16),
            pltpu.VMEM((nz, own, cols), BF16),
            pltpu.VMEM((nz, own, cols), BF16),
            dma((8 + heads,)),
            dma((peers, 2)),
            dma((peers, 2)),
            dma((nz, 2)),
            dma((nz, ny, 2)),
            dma((nz, peers, 2)),
            dma((nz, ny, 2)),
            dma((nz, 2)),
        ],
        compiler_params=pltpu.CompilerParams(collective_id=0, has_side_effects=True),
        name="decode_step",
    )(
        tokens, norm_gain.reshape(1, -1), w_input_gate.T, w_forget_gate.T, normalizer, memory_max.T,
        ffn_gain.reshape(1, cols), w_key, w_value, w_query, w_outgate, memory, w_output, w_gate, w_up, w_down,
    )
    chunk = 2 if own % 2 == 0 else 1
    new_memory, new_normalizer, new_max, result = pl.pallas_call(
        functools.partial(update_kernel, chunk),
        out_shape=(
            jax.ShapeDtypeStruct(memory.shape, F32),
            jax.ShapeDtypeStruct(normalizer.shape, F32),
            jax.ShapeDtypeStruct((heads, own), F32),
            jax.ShapeDtypeStruct(tokens.shape, BF16),
        ),
        in_specs=[ANY, VMEM, VMEM, VMEM, VMEM],
        out_specs=(ANY, VMEM, VMEM, VMEM),
        scratch_shapes=[vm(memory), dma((own // chunk,)), dma((own // chunk,))],
        name="memory_update",
    )(memory, aux, normalizer, new_max, result)
    return (result, new_memory, new_normalizer, new_max.T)


def solution(mesh):
    placed = (
        P("kv", "tp"),
        P(),
        P(None, "tp"),
        P(None, "tp"),
        P(None, "tp"),
        P(None, "tp"),
        P(),
        P(),
        P("kv", "tp", None, None),
        P("kv", "tp", None),
        P("kv", "tp"),
        P(None, "tp"),
        P("tp"),
        P("tp", "kv"),
        P("tp", "kv"),
        P("kv", "tp"),
    )
    return jax.shard_map(
        functools.partial(per_device, mesh),
        mesh=mesh,
        in_specs=placed,
        out_specs=(P("kv", "tp"), P("kv", "tp", None, None), P("kv", "tp", None), P("kv", "tp")),
        check_vma=False,
    )
```
